128 devices in a mesh: sp: 32 (over z, y, core), tp: 4 (over x).
Axes of the slice: x: 4, y: 4, z: 4, core: 2. Of those that a mesh axis runs over, the one named last changes fastest.
Arguments:
- residual_input_stream: bfloat16 [24576, 2048], P('sp'), may hold values from -6 to 6
- projected_queries: bfloat16 [24576, 512], P('sp', 'tp'), may hold values from -6 to 6
- projected_keys: bfloat16 [24576, 512], P('sp', 'tp'), may hold values from -6 to 6
- projected_values: bfloat16 [24576, 1024], P('sp', 'tp'), may hold values from -6 to 6
- emitted_switch_entries: bfloat16 [24576, 1024], P('sp', 'tp'), may hold values from -6 to 6
- retention_preactivations: bfloat16 [24576, 512], P('sp', 'tp'), may hold values from -6 to 15
- additional_fading_amount: float32 [24576], P('sp'), may hold values from -2 to 0
- head_norm_gain: float32 [128], replicated, may hold values from 0.1 to 1.9
- attention_output_weight: bfloat16 [1024, 2048], P('tp'), may hold values from -0.1875 to 0.1875
- feedforward_norm_gain: float32 [2048], replicated, may hold values from 0.1 to 1.9
- gate_up_matrix: bfloat16 [2048, 5632], P('sp', 'tp'), may hold values from -0.125 to 0.125
- value_up_matrix: bfloat16 [2048, 5632], P('sp', 'tp'), may hold values from -0.125 to 0.125
- gate_filter_taps: bfloat16 [3, 5632], P(None, 'tp'), may hold values from -3.5 to 3.5
- value_filter_taps: bfloat16 [3, 5632], P(None, 'tp'), may hold values from -3.5 to 3.5
- down_projection_weight: bfloat16 [5632, 2048], P('tp', 'sp'), may hold values from -0.078125 to 0.078125
Outputs:
- layer_out: bfloat16 [24576, 2048], P(('sp', 'tp'))
The draws below stay inside these ranges and needn't reach their ends.
All inputs are finite; a program needn't handle non-finite values.
Results may differ from the reference program's by a relative error of at most 0.011.
Values may be sent and summed in bfloat16 or wider, within the bound.
A program may use at most 128 MiB of HBM per device.

```python
import math
import jax
import jax.numpy as jnp
from jax import lax

D = 2048
HEADS = 8
DK = 64
DV = 128
FF = 5632
CONV = 3
BLOCK = 64
TOK_DEV = 768
KW = 512
VW = 1024
TOKENS = 24576


def draw_retention_preactivations(key, part):
    keys_all = jax.random.split(jax.random.fold_in(key, 11), 3)
    ranking = jax.random.permutation(keys_all[0], HEADS)
    fast_count = HEADS // 2
    channel_head = jnp.arange(HEADS * DK) // DK
    head_fast = (ranking < fast_count).astype(jnp.float32)
    chan_fast = jnp.sum((channel_head[:, None] == jnp.arange(HEADS)[None, :]).astype(jnp.float32) * head_fast[None, :], axis=1)
    slow_base = math.log(TOKENS) - 1.6
    base = chan_fast + (1.0 - chan_fast) * slow_base
    device_count = TOKENS // TOK_DEV
    shifts = jax.random.uniform(keys_all[1], (device_count,), jnp.float32, -1.0, 1.0)
    position_dev = jnp.arange(TOKENS) // TOK_DEV
    shift_rows = jnp.sum((position_dev[:, None] == jnp.arange(device_count)[None, :]).astype(jnp.float32) * shifts[None, :], axis=1)
    noise = jnp.clip(jax.random.normal(keys_all[2], (TOKENS, HEADS * DK), jnp.float32), -5.0, 5.0)
    return (base[None, :] + shift_rows[:, None] + noise).astype(jnp.bfloat16)


def draw_additional_fading_amount(key, part):
    keys_all = jax.random.split(jax.random.fold_in(key, 23), 2)
    places = jax.random.randint(keys_all[0], (3,), 0, TOKENS)
    depths = jnp.log(jax.random.uniform(keys_all[1], (3,), jnp.float32, 0.5, 0.8))
    marks = (jnp.arange(TOKENS)[:, None] == places[None, :]).astype(jnp.float32)
    return jnp.sum(marks * depths[None, :], axis=1).astype(jnp.float32)


def levels(key, extent, shards, low, top_value):
    level = 1.0
    for position, parts in shards:
        steps = jax.random.uniform(jax.random.fold_in(jax.random.fold_in(key, 6), position), (parts,), jnp.float32, low / len(shards), top_value / len(shards))
        level = level * jnp.repeat(jnp.exp(steps), extent[position] // parts).reshape((-1,) + (1,) * (len(extent) - 1 - position))
    return level


def normal_values(stream_key, shape, scale, reach, pieces=(), kind=jnp.bfloat16):
    entries = jax.random.normal(stream_key, shape, jnp.float32) * scale
    if len(pieces) > 0:
        entries = levels(stream_key, shape, pieces, -0.22, 0.18) * entries
    return jnp.clip(entries, min=-reach, max=reach).astype(kind)


def setup_inputs(seed: int = 0) -> dict:
    seeds = jax.random.split(jax.random.key(seed), 16)
    residual_input_stream = normal_values(seeds[0], (TOKENS, D), 1.0, 6.0, ((0, 32),))
    projected_queries = normal_values(seeds[1], (TOKENS, KW), 1.0, 6.0, ((0, 32), (1, 4)))
    projected_keys = normal_values(seeds[2], (TOKENS, KW), 1.0, 6.0, ((0, 32), (1, 4)))
    projected_values = normal_values(seeds[3], (TOKENS, VW), 1.0, 6.0, ((0, 32), (1, 4)))
    emitted_switch_entries = normal_values(seeds[4], (TOKENS, VW), 1.0, 6.0, ((0, 32), (1, 4)))
    retention_preactivations = draw_retention_preactivations(jax.random.fold_in(seeds[15], 71), 0)
    additional_fading_amount = draw_additional_fading_amount(jax.random.fold_in(seeds[15], 71), 0)
    head_norm_gain = jnp.clip(1.0 + 0.18 * jax.random.normal(seeds[7], (DV,), jnp.float32), 0.1, 1.9)
    attention_output_weight = normal_values(seeds[8], (VW, D), VW ** -0.5, 0.1875, ((0, 4),))
    feedforward_norm_gain = jnp.clip(1.0 + 0.18 * jax.random.normal(seeds[9], (D,), jnp.float32), 0.1, 1.9)
    gate_up_matrix = normal_values(seeds[10], (D, FF), D ** -0.5, 0.125, ((0, 32), (1, 4)))
    value_up_matrix = normal_values(seeds[11], (D, FF), D ** -0.5, 0.125, ((0, 32), (1, 4)))
    gate_filter_taps = normal_values(seeds[12], (CONV, FF), CONV ** -0.5, 3.5, ((1, 4),))
    value_filter_taps = normal_values(seeds[13], (CONV, FF), CONV ** -0.5, 3.5, ((1, 4),))
    down_projection_weight = normal_values(seeds[14], (FF, D), FF ** -0.5, 0.078125, ((0, 4), (1, 32)))
    return dict(residual_input_stream=residual_input_stream, projected_queries=projected_queries, projected_keys=projected_keys, projected_values=projected_values, emitted_switch_entries=emitted_switch_entries, retention_preactivations=retention_preactivations, additional_fading_amount=additional_fading_amount, head_norm_gain=head_norm_gain, attention_output_weight=attention_output_weight, feedforward_norm_gain=feedforward_norm_gain, gate_up_matrix=gate_up_matrix, value_up_matrix=value_up_matrix, gate_filter_taps=gate_filter_taps, value_filter_taps=value_filter_taps, down_projection_weight=down_projection_weight)


eps = 1e-06
retention_sharpness = 16.0

def to_blocks(tensor, width):
    count = tensor.shape[0] // BLOCK
    return tensor.astype(jnp.float32).reshape(count, BLOCK, HEADS, width)

def depthwise(upward, taps):
    length = upward.shape[0]
    padded = jnp.concatenate([jnp.zeros((CONV - 1, upward.shape[1]), jnp.bfloat16), upward], axis=0)
    result = jnp.zeros(upward.shape, jnp.float32)
    for offset in range(CONV):
        result = result + taps[offset].astype(jnp.float32)[None] * padded[offset:offset + length].astype(jnp.float32)
    return result

def reference(residual_input_stream, projected_queries, projected_keys, projected_values, emitted_switch_entries, retention_preactivations, additional_fading_amount, head_norm_gain, attention_output_weight, feedforward_norm_gain, gate_up_matrix, value_up_matrix, gate_filter_taps, value_filter_taps, down_projection_weight):
    largest_exponent = lax.Precision.HIGHEST
    retention_logarithm = jax.nn.log_sigmoid(retention_preactivations.astype(jnp.float32)) / retention_sharpness + additional_fading_amount[:, None]
    scaled_q = to_blocks(projected_queries, DK) * DK ** (-0.5)
    key_heads = to_blocks(projected_keys, DK)
    value_heads = to_blocks(projected_values, DV)
    rate_cum = jnp.cumsum(to_blocks(retention_logarithm, DK), axis=1)
    block_total = rate_cum[:, -1]
    q_decayed = scaled_q * jnp.exp(rate_cum)
    k_growth = key_heads * jnp.exp(-rate_cum)
    fading_through_finish = key_heads * jnp.exp(block_total[:, None] - rate_cum)
    lower = jnp.tril(jnp.ones((BLOCK, BLOCK), bool))
    scores = jnp.einsum('nihk,njhk->nhij', q_decayed, k_growth, precision=largest_exponent)
    scores = jnp.where(lower[None, None], scores, 0.0)
    within = jnp.einsum('nhij,njhv->nihv', scores, value_heads, precision=largest_exponent)
    increments = jnp.einsum('nchk,nchv->nhkv', fading_through_finish, value_heads, precision=largest_exponent)

    def advance_recurrence(state, inputs):
        factor, increment = inputs
        return (factor[..., None] * state + increment, state)
    start_state = jnp.zeros((HEADS, DK, DV), jnp.float32)
    final_state, state_before = lax.scan(advance_recurrence, start_state, (jnp.exp(block_total), increments))
    earlier = jnp.einsum('nchk,nhkv->nchv', q_decayed, state_before, precision=largest_exponent)
    mech_out = (within + earlier).reshape(TOKENS, HEADS, DV)
    mech_out = mech_out * lax.rsqrt(lax.optimization_barrier(jnp.mean(mech_out * mech_out, axis=-1, keepdims=True)) + eps) * head_norm_gain
    mixed = (mech_out.reshape(TOKENS, VW) * jax.nn.silu(emitted_switch_entries.astype(jnp.float32))).astype(jnp.bfloat16)
    attended = jnp.dot(mixed, attention_output_weight, preferred_element_type=jnp.float32)
    resid = residual_input_stream.astype(jnp.float32) + attended
    normed = (resid * lax.rsqrt(lax.optimization_barrier(jnp.mean(resid * resid, axis=-1, keepdims=True)) + eps) * feedforward_norm_gain).astype(jnp.bfloat16)
    gate_up = jnp.dot(normed, gate_up_matrix, preferred_element_type=jnp.float32).astype(jnp.bfloat16)
    value_up = jnp.dot(normed, value_up_matrix, preferred_element_type=jnp.float32).astype(jnp.bfloat16)
    gate_mix = depthwise(gate_up, gate_filter_taps)
    value_mix = depthwise(value_up, value_filter_taps)
    hidden = (jax.nn.silu(gate_mix) * value_mix).astype(jnp.bfloat16)
    return (resid + jnp.dot(hidden, down_projection_weight, preferred_element_type=jnp.float32)).astype(jnp.bfloat16)
```

```python
import jax
import jax.numpy as jnp
from jax import lax
from jax.experimental import pallas as pl
from jax.experimental.pallas import tpu as pltpu
from jax.sharding import Mesh
from jax.sharding import PartitionSpec as P

MESH = pl.DeviceIdType.MESH
BLOCK = 64
SP = ("sp_0", "sp_1", "sp_2")
EPS = 1e-06
BF = jnp.bfloat16
F32 = jnp.float32

ROWS = 768
D = 2048
HID = 1408
CH = 192
NCH = 4
NB = ROWS // BLOCK
WCOLS = 3 * HID
HALO = 16
NT = HID // 128
CHUNKS = (3, 0, 1, 2)


def wrap(v):
    return lax.rem(v + 8, 4)


def rows_of(start, size):
    return pl.ds(pl.multiple_of(start, 16), size)


def nt_dot(a, b):
    return lax.dot_general(a, b, (((1,), (1,)), ((), ())), preferred_element_type=F32)


def tn_dot(a, b):
    return lax.dot_general(a, b, (((0,), (0,)), ((), ())), preferred_element_type=F32)


def body(
    x_hbm, q_hbm, k_hbm, v_hbm, g_hbm, lr_hbm, wo_hbm, w_hbm, hg_ref, fg_ref, taps_ref,
    out_ref,
    wbuf, wobuf, xbuf, qbuf, kbuf, vbuf, gbuf, lrbuf, tst, cbs, qst, outl,
    cbuf, ybuf, zbuf, mix, normed, resid, own, hid, parts, relay, fin,
    lsem, wsend, wrecv, dsend, drecv, osend, orecv, odsend, odrecv,
    csem, ysend, yrecv, zsend, zrecv, msend, mrecv, hsem, psend, precv,
):
    z, y, c, x = (lax.axis_index(n) for n in ("sp_0", "sp_1", "sp_2", "tp"))
    sp = z * 8 + y * 2 + c
    peer = 1 - c
    spn = lax.rem(sp + 1, 32)
    spp = lax.rem(sp + 31, 32)

    def at_sp(s):
        return {"sp_0": s // 8, "sp_1": lax.rem(s, 8) // 2, "sp_2": lax.rem(s, 2), "tp": x}

    def dev(dz=None, dy=None, dc=None, dx=None):
        return {
            "sp_0": z if dz is None else dz,
            "sp_1": y if dy is None else dy,
            "sp_2": c if dc is None else dc,
            "tp": x if dx is None else dx,
        }

    def remote(src, dst, ssem, rsem, to):
        return pltpu.make_async_remote_copy(
            src_ref=src, dst_ref=dst, send_sem=ssem, recv_sem=rsem, device_id=to,
            device_id_type=MESH,
        )

    wl = pltpu.make_async_copy(w_hbm, wbuf.at[rows_of(sp * 64, 64), :], lsem.at[0])
    wol = pltpu.make_async_copy(wo_hbm, wobuf.at[rows_of(x * 256, 256), :], lsem.at[1])
    loads = [
        pltpu.make_async_copy(a, b, lsem.at[2 + i])
        for i, (a, b) in enumerate(
            ((lr_hbm, lrbuf), (k_hbm, kbuf), (v_hbm, vbuf), (q_hbm, qbuf), (g_hbm, gbuf), (x_hbm, xbuf))
        )
    ]
    wl.start()
    wol.start()
    for cp in loads:
        cp.start()

    barrier = pltpu.get_barrier_semaphore()
    partners = [dev(dc=peer), at_sp(spn), at_sp(spp)]
    partners += [dev(dx=wrap(x + 1)), dev(dx=wrap(x - 1))]
    for dlt in (1, 2, 3):
        partners += [dev(dy=wrap(y + dlt)), dev(dz=wrap(z + dlt))]
    for to in partners:
        pl.semaphore_signal(barrier, inc=1, device_id=to, device_id_type=MESH)
    pl.semaphore_wait(barrier, len(partners))

    def wgeom(t):
        first = 1 - t // 2
        second = t // 2
        s = 1 - 2 * lax.rem(t, 2)
        p = first * y + second * z
        q = first * z + second * y

        def block(pp, qq):
            zz = first * qq + second * pp
            yy = first * pp + second * qq
            return wbuf.at[rows_of((zz * 8 + yy * 2 + c) * 64 + t * 16, 16), :]

        def to_p(dlt):
            return dev(dz=wrap(z + second * dlt), dy=wrap(y + first * dlt))

        def to_q(dlt):
            return dev(dz=wrap(z + first * dlt), dy=wrap(y + second * dlt))

        return s, p, q, block, to_p, to_q

    def wcopy(t, k):
        s, p, q, block, to_p, to_q = wgeom(t)
        if k < 3:
            blk = (block(p, q), block(p, q), block(wrap(p - s), q))[k]
            to = (to_p(1), to_p(-1), to_p(s))[k]
        else:
            m, j = divmod(k - 3, 3)
            pm = wrap(p + (0, -1, 1, 2)[m])
            blk = (block(pm, q), block(pm, q), block(pm, wrap(q - s)))[j]
            to = (to_q(1), to_q(-1), to_q(s))[j]
        return remote(blk, blk, wsend.at[t, k], wrecv.at[t, k], to)

    def wdone(t, k):
        s, p, q, block, to_p, to_q = wgeom(t)
        if k < 3:
            blk = (block(wrap(p - 1), q), block(wrap(p + 1), q), block(wrap(p + 2), q))[k]
        else:
            m, j = divmod(k - 3, 3)
            pm = wrap(p + (0, -1, 1, 2)[m])
            blk = block(pm, wrap(q + (-1, 1, 2)[j]))
        return blk

    def wstep(waits, sends):
        def one(t, carry):
            for k in waits:
                blk = wdone(t, k)
                remote(blk, blk, wsend.at[t, k], wrecv.at[t, k], dev(dc=peer)).wait_recv()
                remote(blk, blk, dsend.at[t, k], drecv.at[t, k], dev(dc=peer)).start()
            for k in sends:
                wcopy(t, k).start()
            return carry

        lax.fori_loop(0, 4, one, 0)

    own_rows = wbuf.at[rows_of(sp * 64, 64), :]
    peer_rows = wbuf.at[rows_of((sp - c + peer) * 64, 64), :]

    wl.wait()
    wstep((), (0, 1))
    own_peer = remote(own_rows, own_rows, csem.at[2], csem.at[3], dev(dc=peer))
    own_peer.start()

    def ohalf(xx, cc):
        return wobuf.at[rows_of(xx * 256 + cc * 128, 128), :]

    def oquart(xx, cc, h):
        return wobuf.at[rows_of(xx * 256 + cc * 128 + h * 64, 64), :]

    xr, xl, xo = wrap(x + 1), wrap(x - 1), wrap(x + 2)
    wol.wait()
    o0 = remote(ohalf(x, c), ohalf(x, c), osend.at[0], orecv.at[0], dev(dx=xr))
    o1 = remote(ohalf(x, c), ohalf(x, c), osend.at[1], orecv.at[1], dev(dx=xl))
    o0.start()
    o1.start()

    lane = lax.broadcasted_iota(jnp.int32, (1, 128), 1)
    low = lane < 64
    ri = lax.broadcasted_iota(jnp.int32, (64, 64), 0)
    ci = lax.broadcasted_iota(jnp.int32, (64, 64), 1)
    tri = (ri >= ci).astype(F32)
    for cp in loads[:3]:
        cp.wait()

    def state_step(n, carry):
        st, cb = carry
        rows = rows_of(n * 64, 64)
        rc = jnp.dot(tri, lrbuf[rows, :], precision=lax.Precision.HIGHEST, preferred_element_type=F32)
        lrbuf[rows, :] = rc
        bt = rc[63:64, :]
        kf = (kbuf[rows, :].astype(F32) * jnp.exp(bt - rc)).astype(BF)
        pr = tn_dot(vbuf[rows, :], kf)
        tst[n] = st
        cbs[n] = jnp.broadcast_to(cb, (8, 128))
        st = jnp.exp(bt) * st + jnp.where(low, pr[:128], pr[128:])
        return st, cb + bt

    st, la = lax.fori_loop(
        0, NB, state_step, (jnp.zeros((128, 128), F32), jnp.zeros((1, 128), F32))
    )

    def put_state(ref, s_, l_):
        ref[0:128, :] = s_
        ref[128:136, :] = jnp.broadcast_to(l_, (8, 128))

    put_state(cbuf.at[0], st, la)
    cx = remote(cbuf.at[0], cbuf.at[1], csem.at[0], csem.at[1], dev(dc=peer))
    cx.start()
    for cp in loads[3:4]:
        cp.wait()

    def within_step(n, carry):
        rows = rows_of(n * 64, 64)
        rc = lrbuf[rows, :]
        qd = qbuf[rows, :].astype(F32) * 0.125 * jnp.exp(rc)
        kg = (kbuf[rows, :].astype(F32) * jnp.exp(-rc)).astype(BF)
        zero = jnp.zeros_like(qd)
        qq = jnp.concatenate([jnp.where(low, qd, zero), jnp.where(low, zero, qd)], axis=0).astype(BF)
        qst[n] = qq
        sc = nt_dot(qq, kg)
        s0 = jnp.where(ri >= ci, sc[:64], 0.0).astype(BF)
        s1 = jnp.where(ri >= ci, sc[64:], 0.0).astype(BF)
        vv = vbuf[rows, :]
        outl[rows, 0:128] = jnp.dot(s0, vv[:, :128], preferred_element_type=F32)
        outl[rows, 128:256] = jnp.dot(s1, vv[:, 128:], preferred_element_type=F32)
        return carry

    lax.fori_loop(0, 3, within_step, 0)
    cx.wait()
    other = cbuf[1, 0:128, :]
    ola = cbuf[1, 128:129, :]
    second = c == 1
    s_first = jnp.where(second, other, st)
    s_second = jnp.where(second, st, other)
    la_second = jnp.where(second, la, ola)
    pc = jnp.where(second, other, jnp.zeros_like(other))
    pc_la = jnp.where(second, ola, jnp.zeros_like(ola))
    chip = jnp.exp(la_second) * s_first + s_second
    chip_la = la + ola

    def ring_scan(buf, ssem, rsem, me, value, value_la, to, cover):
        put_state(buf.at[me], value, value_la)
        sent = [
            remote(buf.at[me], buf.at[me], ssem.at[dlt - 1], rsem.at[dlt - 1], to(wrap(me + dlt)))
            for dlt in (1, 2, 3)
        ]
        for cp in sent:
            cp.start()
        cover()
        for dlt in (1, 2, 3):
            src = buf.at[wrap(me - dlt)]
            remote(src, src, ssem.at[dlt - 1], rsem.at[dlt - 1], to(wrap(me + dlt))).wait_recv()
        tot = jnp.zeros((128, 128), F32)
        tot_la = jnp.zeros((1, 128), F32)
        pre, pre_la = tot, tot_la
        for k in range(4):
            lk = buf[k, 128:129, :]
            tot = jnp.exp(lk) * tot + buf[k, 0:128, :]
            tot_la = tot_la + lk
            passed = k < me
            pre = jnp.where(passed, tot, pre)
            pre_la = jnp.where(passed, tot_la, pre_la)
        return pre, pre_la, tot, tot_la, sent

    py, py_la, tot, tot_la, ysent = ring_scan(
        ybuf, ysend, yrecv, y, chip, chip_la, lambda k: dev(dy=k),
        lambda: lax.fori_loop(3, 6, within_step, 0),
    )
    pz, pz_la, tot, tot_la, zsent = ring_scan(
        zbuf, zsend, zrecv, z, tot, tot_la, lambda k: dev(dz=k),
        lambda: lax.fori_loop(6, 10, within_step, 0),
    )
    tin = jnp.exp(pc_la) * (jnp.exp(py_la) * pz + py) + pc

    wstep((0, 1), (2, 3, 4, 6, 7, 9, 10))
    remote(ohalf(xl, c), ohalf(xl, c), osend.at[0], orecv.at[0], dev(dx=xr)).wait_recv()
    remote(ohalf(xr, c), ohalf(xr, c), osend.at[1], orecv.at[1], dev(dx=xl)).wait_recv()
    o2 = remote(oquart(xl, c, 0), oquart(xl, c, 0), osend.at[2], orecv.at[2], dev(dx=xr))
    o3 = remote(oquart(xr, c, 1), oquart(xr, c, 1), osend.at[3], orecv.at[3], dev(dx=xl))
    o2.start()
    o3.start()
    od = [
        remote(r, r, odsend.at[i], odrecv.at[i], dev(dc=peer))
        for i, r in enumerate((ohalf(xl, c), ohalf(xr, c), oquart(xo, c, 0), oquart(xo, c, 1)))
    ]
    od[0].start()
    od[1].start()
    lax.fori_loop(10, 12, within_step, 0)
    loads[4].wait()

    mlane = pl.multiple_of(x * 256, 256)

    def mix_step(n, carry):
        rows = rows_of(n * 64, 64)
        full = (tst[n] + jnp.exp(cbs[n][0:1, :]) * tin).astype(BF)
        e = nt_dot(qst[n], full)
        got = []
        for h in range(2):
            o = outl[rows, h * 128 : h * 128 + 128] + e[h * 64 : h * 64 + 64]
            o = o * lax.rsqrt(jnp.mean(o * o, axis=-1, keepdims=True) + EPS) * hg_ref[...]
            gt = gbuf[rows, h * 128 : h * 128 + 128].astype(F32)
            got.append(o * (gt / (1.0 + jnp.exp(-gt))))
        mix[rows, pl.ds(mlane, 256)] = jnp.concatenate(got, axis=1).astype(BF)
        return carry

    def mblock(h, xx):
        return mix.at[h * CH : h * CH + CH, pl.ds(pl.multiple_of(xx * 256, 256), 256)]

    msent = []
    for h in CHUNKS:
        lax.fori_loop(h * 3, h * 3 + 3, mix_step, 0)
        for j, to in ((0, xr), (1, xl)):
            cp = remote(mblock(h, x), mblock(h, x), msend.at[h, j], mrecv.at[h, j], dev(dx=to))
            cp.start()
            msent.append(cp)

    def mwait(h, j, xx):
        remote(mblock(h, xx), mblock(h, xx), msend.at[h, j], mrecv.at[h, j], dev(dx=xr)).wait_recv()

    wstep((3, 4, 2), (5, 12, 13))
    for h in CHUNKS:
        mwait(h, 0, xl)
        mwait(h, 1, xr)
        src, to = (xl, xr) if h % 2 == 0 else (xr, xl)
        cp = remote(mblock(h, src), mblock(h, src), msend.at[h, 2], mrecv.at[h, 2], dev(dx=to))
        cp.start()
        msent.append(cp)

    wstep((6, 7, 9, 10), (8, 11))
    remote(oquart(xo, c, 0), oquart(xo, c, 0), osend.at[2], orecv.at[2], dev(dx=xr)).wait_recv()
    remote(oquart(xo, c, 1), oquart(xo, c, 1), osend.at[3], orecv.at[3], dev(dx=xl)).wait_recv()
    od[2].start()
    od[3].start()
    for i, r in enumerate((ohalf(xl, peer), ohalf(xr, peer), oquart(xo, peer, 0), oquart(xo, peer, 1))):
        remote(r, r, odsend.at[i], odrecv.at[i], dev(dc=peer)).wait_recv()
    loads[5].wait()

    def chunk_norm(h):
        r0 = h * CH

        def cols(i, ss):
            cs = pl.ds(pl.multiple_of(i * 256, 256), 256)
            a = jnp.dot(mix[r0 : r0 + CH, :], wobuf[:, cs], preferred_element_type=F32)
            a = a + xbuf[r0 : r0 + CH, cs].astype(F32)
            resid[:, cs] = a
            sq = a * a
            return ss + sq[:, :128] + sq[:, 128:]

        ss = lax.fori_loop(0, 8, cols, jnp.zeros((CH, 128), F32))
        rs = lax.rsqrt(jnp.sum(ss, axis=-1, keepdims=True) * (1.0 / D) + EPS)

        def norm(i, carry):
            cs = pl.ds(pl.multiple_of(i * 256, 256), 256)
            normed[HALO + r0 : HALO + r0 + CH, cs] = (resid[:, cs] * rs * fg_ref[:, cs]).astype(BF)
            return carry

        lax.fori_loop(0, 8, norm, 0)

        @pl.when(x == h)
        def _():
            def keep(i, carry):
                cs = pl.ds(pl.multiple_of(i * 256, 256), 256)
                own[:, cs] = resid[:, cs]
                return carry

            lax.fori_loop(0, 8, keep, 0)

    tail = normed.at[ROWS : ROWS + HALO, :]
    halo = normed.at[0:HALO, :]
    hcopy = remote(tail, halo, hsem.at[0], hsem.at[1], at_sp(spn))
    for h in CHUNKS:
        mwait(h, 2, xo)
        chunk_norm(h)
        if h == 3:
            hcopy.start()
        if h == 1:
            wstep((12, 13), (14,))
    wstep((5, 8, 11), ())
    wstep((14,), ())
    hcopy.wait()

    @pl.when(sp == 0)
    def _():
        normed[0:HALO, :] = jnp.zeros((HALO, D), BF)

    own_peer_in = remote(peer_rows, peer_rows, csem.at[2], csem.at[3], dev(dc=peer))
    own_peer_in.wait_recv()

    def dwait(t, carry):
        for k in range(15):
            blk = wdone(t, k)
            remote(blk, blk, dsend.at[t, k], drecv.at[t, k], dev(dc=peer)).wait_recv()
        return carry

    lax.fori_loop(0, 4, dwait, 0)

    half = D // 2

    def ffn_chunk(i, carry):
        off = 2 - i + 3 * (i // 2) - 2 * (i // 3)
        h = lax.rem(x + off, 4)
        r0 = h * CH
        win = rows_of(r0, CH + HALO)

        def up(j, cc):
            cs = pl.ds(pl.multiple_of(j * 256, 256), 256)
            u = jnp.dot(normed[win, :], wbuf[:, cs], preferred_element_type=F32)
            u = u.astype(BF).astype(F32)
            t0, t1, t2 = (taps_ref[a : a + 1, cs] for a in range(3))
            m = t0 * pltpu.roll(u, 2, 0) + t1 * pltpu.roll(u, 1, 0) + t2 * u
            gm = m[HALO:, :128]
            vm = m[HALO:, 128:]
            hv = gm / (1.0 + jnp.exp(-gm)) * vm
            hid[:, pl.ds(pl.multiple_of(j * 128, 128), 128)] = hv.astype(BF)
            return cc

        lax.fori_loop(0, NT, up, 0)

        def down(j, cc):
            rs_ = rows_of(j * 256, 256)
            a = nt_dot(hid[...], wbuf[rs_, 2 * HID : WCOLS])
            parts[i, :, pl.ds(pl.multiple_of(j * 256, 256), 256)] = a.astype(BF)
            return cc

        lax.fori_loop(0, 8, down, 0)

        @pl.when(i == 0)
        def _():
            remote(parts.at[0, :, 0:half], relay.at[0], psend.at[0], precv.at[0], dev(dx=xr)).start()
            remote(parts.at[0, :, half:D], relay.at[1], psend.at[1], precv.at[1], dev(dx=xl)).start()

        @pl.when(i == 1)
        def _():
            remote(parts.at[1, :, half:D], fin.at[0, :, half:D], psend.at[2], precv.at[2], dev(dx=xr)).start()

        @pl.when(i == 2)
        def _():
            remote(parts.at[2, :, 0:half], fin.at[1, :, 0:half], psend.at[3], precv.at[3], dev(dx=xl)).start()

        return carry

    lax.fori_loop(0, NCH, ffn_chunk, 0)

    def add_relay(slot, ref, base):
        def one(j, cc):
            a = pl.ds(pl.multiple_of(j * 256, 256), 256)
            b = pl.ds(pl.multiple_of(base + j * 256, 256), 256)
            parts[slot, :, b] = (parts[slot, :, b].astype(F32) + ref[:, a].astype(F32)).astype(BF)
            return cc

        lax.fori_loop(0, 4, one, 0)

    r0c = remote(parts.at[0, :, 0:half], relay.at[0], psend.at[0], precv.at[0], dev(dx=xr))
    r1c = remote(parts.at[0, :, half:D], relay.at[1], psend.at[1], precv.at[1], dev(dx=xl))
    r0c.wait_recv()
    add_relay(1, relay.at[0], 0)
    f0 = remote(parts.at[1, :, 0:half], fin.at[0, :, 0:half], psend.at[4], precv.at[4], dev(dx=xr))
    f0.start()
    r1c.wait_recv()
    add_relay(2, relay.at[1], half)
    f1 = remote(parts.at[2, :, half:D], fin.at[1, :, half:D], psend.at[5], precv.at[5], dev(dx=xl))
    f1.start()

    def sends_over(t, carry):
        for k in range(15):
            wcopy(t, k).wait_send()
            blk = wdone(t, k)
            remote(blk, blk, dsend.at[t, k], drecv.at[t, k], dev(dc=peer)).wait_send()
        return carry

    lax.fori_loop(0, 4, sends_over, 0)
    own_peer.wait_send()
    for cp in (o0, o1, o2, o3, *od, *ysent, *zsent, *msent):
        cp.wait_send()

    g0 = remote(parts.at[1, :, half:D], fin.at[0, :, half:D], psend.at[2], precv.at[2], dev(dx=xr))
    g1 = remote(parts.at[2, :, 0:half], fin.at[1, :, 0:half], psend.at[3], precv.at[3], dev(dx=xl))
    for cp in (g0, g1, f0, f1):
        cp.wait_recv()

    def last(j, cc):
        cs = pl.ds(pl.multiple_of(j * 256, 256), 256)
        a = own[:, cs] + parts[3, :, cs].astype(F32)
        a = a + (fin[0, :, cs].astype(F32) + fin[1, :, cs].astype(F32))
        out_ref[:, cs] = a.astype(BF)
        return cc

    lax.fori_loop(0, 8, last, 0)
    for cp in (r0c, r1c, g0, g1, f0, f1):
        cp.wait_send()


def per_device(
    residual_input_stream, projected_queries, projected_keys, projected_values,
    emitted_switch_entries, retention_preactivations, additional_fading_amount, head_norm_gain,
    attention_output_weight, feedforward_norm_gain, gate_up_matrix, value_up_matrix,
    gate_filter_taps, value_filter_taps, down_projection_weight,
):
    lr = (
        jax.nn.log_sigmoid(retention_preactivations.astype(F32)) / 16.0
        + additional_fading_amount[:, None]
    )

    def woven(a, b):
        n = a.shape[0]
        both = jnp.stack([a.reshape(n, NT, 128), b.reshape(n, NT, 128)], axis=2)
        return both.reshape(n, 2 * HID)

    w = jnp.concatenate([woven(gate_up_matrix, value_up_matrix), down_projection_weight.T], axis=1)
    taps = woven(gate_filter_taps, value_filter_taps).astype(F32)
    anyspec = pl.BlockSpec(memory_space=pl.ANY)
    vspec = pl.BlockSpec(memory_space=pltpu.VMEM)
    dma = pltpu.SemaphoreType.DMA
    v = pltpu.VMEM
    return pl.pallas_call(
        body,
        out_shape=jax.ShapeDtypeStruct((CH, D), BF),
        in_specs=[anyspec] * 8 + [vspec] * 3,
        out_specs=vspec,
        scratch_shapes=[
            v((D, WCOLS), BF), v((1024, D), BF), v((ROWS, D), BF),
            v((ROWS, 128), BF), v((ROWS, 128), BF), v((ROWS, 256), BF), v((ROWS, 256), BF),
            v((ROWS, 128), F32), v((NB, 128, 128), F32), v((NB, 8, 128), F32),
            v((NB, 128, 128), BF), v((ROWS, 256), F32),
            v((2, 136, 128), F32), v((4, 136, 128), F32), v((4, 136, 128), F32),
            v((ROWS, 1024), BF), v((ROWS + HALO, D), BF), v((CH, D), F32), v((CH, D), F32),
            v((CH, HID), BF), v((4, CH, D), BF), v((2, CH, D // 2), BF), v((2, CH, D), BF),
            dma((8,)), dma((4, 15)), dma((4, 15)), dma((4, 15)), dma((4, 15)),
            dma((4,)), dma((4,)), dma((4,)), dma((4,)),
            dma((4,)), dma((3,)), dma((3,)), dma((3,)), dma((3,)),
            dma((4, 3)), dma((4, 3)), dma((2,)), dma((6,)), dma((6,)),
        ],
        compiler_params=pltpu.CompilerParams(
            collective_id=0, has_side_effects=True, vmem_limit_bytes=62 * 1024 * 1024
        ),
        name="layer",
    )(
        residual_input_stream, projected_queries, projected_keys, projected_values,
        emitted_switch_entries, lr, attention_output_weight, w,
        head_norm_gain[None], feedforward_norm_gain[None], taps,
    )


def solution(mesh):
    torus = Mesh(mesh.devices.reshape(4, 4, 2, mesh.shape["tp"]), (*SP, "tp"))
    return jax.shard_map(
        per_device,
        mesh=torus,
        in_specs=(
            P(SP, None), P(SP, "tp"), P(SP, "tp"), P(SP, "tp"), P(SP, "tp"), P(SP, "tp"),
            P(SP), P(), P("tp", None), P(), P(SP, "tp"), P(SP, "tp"), P(None, "tp"),
            P(None, "tp"), P("tp", SP),
        ),
        out_specs=P((*SP, "tp"), None),
        check_vma=False,
    )
```

```python
import jax
import jax.numpy as jnp
from jax import lax
from jax.experimental import pallas as pl
from jax.experimental.pallas import tpu as pltpu
from jax.sharding import Mesh
from jax.sharding import PartitionSpec as P

MESH = pl.DeviceIdType.MESH
BLOCK = 64
SP = ("sp_0", "sp_1", "sp_2")
EPS = 1e-06
BF = jnp.bfloat16
F32 = jnp.float32

ROWS = 768
D = 2048
HID = 1408
CH = 192
NCH = 4
NB = ROWS // BLOCK
GVW = 2 * HID
MAIN = 1280
HALFK = HID // 2
HALO = 16
OFF = (
    (0, 0), (-1, 0), (1, 0), (0, -1), (0, 1), (-1, -1), (1, 1), (1, -1), (-1, 1),
    (2, -1), (2, 1), (1, 2), (-1, 2), (2, 0), (0, 2), (2, 2),
)
VIA = (
    None, (-1, 0), (1, 0), (0, -1), (0, 1), (-1, 0), (1, 0), (0, -1), (0, 1),
    (-1, 0), (1, 0), (0, -1), (0, 1), (-1, 0), (0, -1), (0, 1),
)
SRC = (None, 0, 0, 0, 0, 3, 4, 2, 1, 5, 6, 7, 8, 1, 3, 10)
MIRROR = (0, 2, 1, 4, 3, 6, 5, 8, 7, 10, 9, 12, 11, 13, 14, 15)
QK = HALFK // 2
NT = HID // 128
STEPS = (
    ((), (1, 2, 3, 4)),
    ((1, 2, 3, 4), (5, 6, 7, 8)),
    ((5, 6, 7, 8), (9, 10, 11, 12, 13, 14)),
    ((9, 10, 11, 12), (15,)),
    ((13, 14, 15), ()),
)
CHUNKS = (3, 0, 1, 2)


def wrap(v):
    return lax.rem(v + 8, 4)


def rows_of(start, size):
    return pl.ds(pl.multiple_of(start, 16), size)


def nt_dot(a, b):
    return lax.dot_general(a, b, (((1,), (1,)), ((), ())), preferred_element_type=F32)


def tn_dot(a, b):
    return lax.dot_general(a, b, (((0,), (0,)), ((), ())), preferred_element_type=F32)


def body(
    x_hbm, q_hbm, k_hbm, v_hbm, g_hbm, r_hbm, wo_hbm, gw_hbm, vw_hbm, dw_hbm,
    fade_ref, hg_ref, fg_ref, gt_ref, vt_ref,
    out_ref,
    wgv, dbuf, dloc, dex, wobuf, xbuf, qbuf, kbuf, vbuf, gbuf, rbuf, rcb, tst, cbs, qst, outl,
    cbuf, ybuf, zbuf, mix, normed, resid, own, hid, parts, relay, fin,
    lsem, wsend, wrecv, dsend, drecv, osend, orecv, odsend, odrecv,
    csem, ysend, yrecv, zsend, zrecv, msend, mrecv, hsem, psend, precv,
):
    z, y, c, x = (lax.axis_index(n) for n in ("sp_0", "sp_1", "sp_2", "tp"))
    sp = z * 8 + y * 2 + c
    peer = 1 - c
    spn = lax.rem(sp + 1, 32)
    spp = lax.rem(sp + 31, 32)
    xr, xl, xo = wrap(x + 1), wrap(x - 1), wrap(x + 2)

    def at_sp(s):
        return {"sp_0": s // 8, "sp_1": lax.rem(s, 8) // 2, "sp_2": lax.rem(s, 2), "tp": x}

    def dev(dz=None, dy=None, dc=None, dx=None):
        return {
            "sp_0": z if dz is None else dz,
            "sp_1": y if dy is None else dy,
            "sp_2": c if dc is None else dc,
            "tp": x if dx is None else dx,
        }

    def remote(src, dst, ssem, rsem, to):
        return pltpu.make_async_remote_copy(
            src_ref=src, dst_ref=dst, send_sem=ssem, recv_sem=rsem, device_id=to,
            device_id_type=MESH,
        )

    barrier = pltpu.get_barrier_semaphore()
    partners = [dev(dc=peer), at_sp(spn), at_sp(spp), dev(dx=xr), dev(dx=xl)]
    for dlt in (1, 2, 3):
        partners += [dev(dy=wrap(y + dlt)), dev(dz=wrap(z + dlt))]
    for to in partners:
        pl.semaphore_signal(barrier, inc=1, device_id=to, device_id_type=MESH)

    mine = rows_of(sp * 64, 64)
    pairs = [
        (r_hbm, rbuf), (k_hbm, kbuf), (v_hbm, vbuf),
        (gw_hbm.at[:, 0:MAIN], wgv.at[mine, 0:MAIN]),
        (vw_hbm.at[:, 0:MAIN], wgv.at[mine, MAIN : 2 * MAIN]),
        (gw_hbm.at[:, MAIN:HID], wgv.at[mine, 2 * MAIN : 2 * MAIN + 128]),
        (vw_hbm.at[:, MAIN:HID], wgv.at[mine, 2 * MAIN + 128 : GVW]),
        (wo_hbm, wobuf.at[rows_of(x * 256, 256), :]),
        (dw_hbm, dloc), (q_hbm, qbuf), (g_hbm, gbuf), (x_hbm, xbuf),
    ]
    loads = [pltpu.make_async_copy(a, b, lsem.at[i]) for i, (a, b) in enumerate(pairs)]
    for cp in loads:
        cp.start()

    def shifted(off):
        dz, dy = off
        return wrap(z + dz), wrap(y + dy)

    def wref(pc, slot, cc):
        if pc >= 2:
            col = slot if pc == 2 else MIRROR[slot]
            return dbuf.at[rows_of(cc * HALFK + (pc - 2) * QK, QK), col * 128 : col * 128 + 128]
        dz, dy = OFF[slot]
        zz, yy = shifted((dz, dy) if pc == 0 else (-dz, -dy))
        return wgv.at[rows_of((zz * 8 + yy * 2 + cc) * 64 + pc * 32, 32), :]

    def wsendto(pc, r):
        vz, vy = VIA[r]
        src_slot = SRC[r]
        if pc >= 2 and r == 15:
            vz, vy = 1, 0
            src_slot = 11
        if pc % 2 == 1:
            vz, vy = -vz, -vy
        zz, yy = shifted((-vz, -vy))
        src = wref(pc, src_slot, c)
        dst = wref(pc, r, c) if pc >= 2 else src
        return remote(src, dst, wsend.at[pc, r], wrecv.at[pc, r], dev(dz=zz, dy=yy))

    def wpeer(pc, slot, cc):
        blk = wref(pc, slot, cc)
        return remote(blk, blk, dsend.at[pc, slot], drecv.at[pc, slot], dev(dc=peer))

    def wstep(pc, e):
        waits, sends = STEPS[e]
        for r in waits:
            blk = wref(pc, r, c)
            remote(blk, blk, wsend.at[pc, r], wrecv.at[pc, r], dev(dc=peer)).wait_recv()
        for r in sends:
            wsendto(pc, r).start()
        for r in waits or ((0,) if pc < 2 else ()):
            wpeer(pc, r, c).start()

    def ohalf(xx, cc):
        return wobuf.at[rows_of(xx * 256 + cc * 128, 128), :]

    def oquart(xx, cc, h):
        return wobuf.at[rows_of(xx * 256 + cc * 128 + h * 64, 64), :]

    lane = lax.broadcasted_iota(jnp.int32, (1, 128), 1)
    low = lane < 64
    ri = lax.broadcasted_iota(jnp.int32, (64, 64), 0)
    ci = lax.broadcasted_iota(jnp.int32, (64, 64), 1)
    li = lax.broadcasted_iota(jnp.int32, (64, 128), 1) - lax.broadcasted_iota(jnp.int32, (64, 128), 0)
    tri = (ri >= ci).astype(F32)
    for cp in loads[:3]:
        cp.wait()

    def state_step(n, carry):
        st, cb = carry
        rows = rows_of(n * 64, 64)
        fr = jnp.where(li == 64 * lax.rem(n, 2), fade_ref[pl.ds(n // 2, 1), :], 0.0)
        r = rbuf[rows, :].astype(F32)
        soft = jnp.maximum(-r, 0.0) + jnp.log1p(jnp.exp(-jnp.abs(r)))
        lr = jnp.sum(fr, axis=-1, keepdims=True) - soft * (1.0 / 16.0)
        rc = jnp.dot(tri, lr, precision=lax.Precision.HIGHEST, preferred_element_type=F32)
        rcb[rows, :] = rc
        bt = rc[63:64, :]
        kf = (kbuf[rows, :].astype(F32) * jnp.exp(bt - rc)).astype(BF)
        pr = tn_dot(vbuf[rows, :], kf)
        tst[n] = st
        cbs[n] = jnp.broadcast_to(cb, (8, 128))
        st = jnp.exp(bt) * st + jnp.where(low, pr[:128], pr[128:])
        return st, cb + bt

    def states(first, carry):
        for n in range(4):
            carry = state_step(first + n, carry)
        return carry

    carry = states(0, (jnp.zeros((128, 128), F32), jnp.zeros((1, 128), F32)))
    pl.semaphore_wait(barrier, len(partners))
    for cp in loads[3:7]:
        cp.wait()
    wstep(0, 0)
    loads[7].wait()
    o0 = remote(ohalf(x, c), ohalf(x, c), osend.at[0], orecv.at[0], dev(dx=xr))
    o1 = remote(ohalf(x, c), ohalf(x, c), osend.at[1], orecv.at[1], dev(dx=xl))
    o0.start()
    o1.start()
    st, la = lax.fori_loop(1, 3, lambda i, a: states(4 * i, a), carry)
    def put_state(ref, s_, l_):
        ref[0:128, :] = s_.astype(BF)
        hi = l_.astype(BF).astype(F32)
        mid = (l_ - hi).astype(BF).astype(F32)
        rr = lax.broadcasted_iota(jnp.int32, (16, 128), 0)
        ref[128:144, :] = jnp.where(
            rr == 0, hi, jnp.where(rr == 1, mid, jnp.where(rr == 2, l_ - hi - mid, 0.0))
        ).astype(BF)

    def get_state(ref):
        return ref[0:128, :].astype(F32), jnp.sum(ref[128:144, :].astype(F32), axis=0, keepdims=True)

    put_state(cbuf.at[0], st, la)
    cx = remote(cbuf.at[0], cbuf.at[1], csem.at[0], csem.at[1], dev(dc=peer))
    cx.start()
    loads[8].wait()
    dx = remote(dloc, dex, csem.at[2], csem.at[3], dev(dc=peer))
    dx.start()
    loads[9].wait()

    def within_step(n):
        rows = rows_of(n * 64, 64)
        rc = rcb[rows, :]
        qd = qbuf[rows, :].astype(F32) * 0.125 * jnp.exp(rc)
        kg = (kbuf[rows, :].astype(F32) * jnp.exp(-rc)).astype(BF)
        zero = jnp.zeros_like(qd)
        qq = jnp.concatenate([jnp.where(low, qd, zero), jnp.where(low, zero, qd)], axis=0).astype(BF)
        qst[n] = qq
        sc = nt_dot(qq, kg)
        s0 = jnp.where(ri >= ci, sc[:64], 0.0).astype(BF)
        s1 = jnp.where(ri >= ci, sc[64:], 0.0).astype(BF)
        vv = vbuf[rows, :]
        outl[rows, 0:128] = jnp.dot(s0, vv[:, :128], preferred_element_type=F32)
        outl[rows, 128:256] = jnp.dot(s1, vv[:, 128:], preferred_element_type=F32)

    def within(first):
        for n in range(4):
            within_step(first + n)

    within(0)
    cx.wait()
    other, ola = get_state(cbuf.at[1])
    second = c == 1
    s_first = jnp.where(second, other, st)
    s_second = jnp.where(second, st, other)
    la_second = jnp.where(second, la, ola)
    pc = jnp.where(second, other, jnp.zeros_like(other))
    pc_la = jnp.where(second, ola, jnp.zeros_like(ola))
    chip = jnp.exp(la_second) * s_first + s_second
    chip_la = la + ola

    def ring_scan(buf, ssem, rsem, me, value, value_la, to, cover):
        put_state(buf.at[me], value, value_la)
        sent = [
            remote(buf.at[me], buf.at[me], ssem.at[dlt - 1], rsem.at[dlt - 1], to(wrap(me + dlt)))
            for dlt in (1, 2, 3)
        ]
        for cp in sent:
            cp.start()
        cover()
        for dlt in (1, 2, 3):
            src = buf.at[wrap(me - dlt)]
            remote(src, src, ssem.at[dlt - 1], rsem.at[dlt - 1], to(wrap(me + dlt))).wait_recv()
        tot = jnp.zeros((128, 128), F32)
        tot_la = jnp.zeros((1, 128), F32)
        pre, pre_la = tot, tot_la
        for k in range(4):
            tk, lk = get_state(buf.at[k])
            tot = jnp.exp(lk) * tot + tk
            tot_la = tot_la + lk
            passed = k < me
            pre = jnp.where(passed, tot, pre)
            pre_la = jnp.where(passed, tot_la, pre_la)
        return pre, pre_la, tot, tot_la, sent

    def cover_y():
        wstep(1, 0)
        within(4)

    def join_down():
        dx.wait_recv()

        def one(j, cc):
            cs = pl.ds(pl.multiple_of(j * 128, 128), 128)
            a = dloc[:, cs].astype(F32)
            b = dex[:, cs].astype(F32)
            both = jnp.concatenate([jnp.where(c == 1, b, a), jnp.where(c == 1, a, b)], axis=0)
            dbuf[rows_of(j * 128, 128), 0:128] = both.T.astype(BF)
            return cc

        lax.fori_loop(0, NT, one, 0)

    def cover_z():
        wstep(0, 1)
        within(8)
        join_down()

    py, py_la, tot, tot_la, ysent = ring_scan(
        ybuf, ysend, yrecv, y, chip, chip_la, lambda k: dev(dy=k), cover_y
    )
    pz, pz_la, tot, tot_la, zsent = ring_scan(
        zbuf, zsend, zrecv, z, tot, tot_la, lambda k: dev(dz=k), cover_z
    )
    tin = jnp.exp(pc_la) * (jnp.exp(py_la) * pz + py) + pc
    loads[10].wait()

    mlane = pl.multiple_of(x * 256, 256)

    def mix_step(n):
        rows = rows_of(n * 64, 64)
        full = (tst[n] + jnp.exp(cbs[n][0:1, :]) * tin).astype(BF)
        e = nt_dot(qst[n], full)
        got = []
        for h in range(2):
            o = outl[rows, h * 128 : h * 128 + 128] + e[h * 64 : h * 64 + 64]
            o = o * lax.rsqrt(jnp.mean(o * o, axis=-1, keepdims=True) + EPS) * hg_ref[...]
            gt = gbuf[rows, h * 128 : h * 128 + 128].astype(F32)
            got.append(o * (gt / (1.0 + jnp.exp(-gt))))
        mix[rows, pl.ds(mlane, 256)] = jnp.concatenate(got, axis=1).astype(BF)

    def mblock(h, xx):
        return mix.at[h * CH : h * CH + CH, pl.ds(pl.multiple_of(xx * 256, 256), 256)]

    msent = []

    def mix_chunk(h):
        for n in range(3):
            mix_step(h * 3 + n)
        for j, to in ((0, xr), (1, xl)):
            cp = remote(mblock(h, x), mblock(h, x), msend.at[h, j], mrecv.at[h, j], dev(dx=to))
            cp.start()
            msent.append(cp)

    def mwait(h, j, xx):
        remote(mblock(h, xx), mblock(h, xx), msend.at[h, j], mrecv.at[h, j], dev(dx=xr)).wait_recv()

    def mrelay(h):
        mwait(h, 0, xl)
        mwait(h, 1, xr)
        src, to = (xl, xr) if h % 2 == 0 else (xr, xl)
        cp = remote(mblock(h, src), mblock(h, src), msend.at[h, 2], mrecv.at[h, 2], dev(dx=to))
        cp.start()
        msent.append(cp)

    mix_chunk(3)
    mix_chunk(0)
    wstep(1, 1)
    remote(ohalf(xl, c), ohalf(xl, c), osend.at[0], orecv.at[0], dev(dx=xr)).wait_recv()
    o2 = remote(oquart(xl, c, 0), oquart(xl, c, 0), osend.at[2], orecv.at[2], dev(dx=xr))
    o2.start()
    remote(ohalf(xr, c), ohalf(xr, c), osend.at[1], orecv.at[1], dev(dx=xl)).wait_recv()
    o3 = remote(oquart(xr, c, 1), oquart(xr, c, 1), osend.at[3], orecv.at[3], dev(dx=xl))
    o3.start()
    od = [
        remote(r, r, odsend.at[i], odrecv.at[i], dev(dc=peer))
        for i, r in enumerate((ohalf(xl, c), ohalf(xr, c), oquart(xo, c, 0), oquart(xo, c, 1)))
    ]
    od[0].start()
    od[1].start()
    wstep(0, 2)
    mrelay(3)
    mrelay(0)
    mix_chunk(1)
    mix_chunk(2)
    wstep(1, 2)
    remote(oquart(xo, c, 0), oquart(xo, c, 0), osend.at[2], orecv.at[2], dev(dx=xr)).wait_recv()
    od[2].start()
    remote(oquart(xo, c, 1), oquart(xo, c, 1), osend.at[3], orecv.at[3], dev(dx=xl)).wait_recv()
    od[3].start()
    wstep(0, 3)
    wstep(2, 0)
    for i, r in enumerate((ohalf(xl, peer), ohalf(xr, peer), oquart(xo, peer, 0), oquart(xo, peer, 1))):
        remote(r, r, odsend.at[i], odrecv.at[i], dev(dc=peer)).wait_recv()
    loads[11].wait()

    def chunk_norm(h):
        r0 = h * CH
        ss = jnp.zeros((CH, 128), F32)
        for i in range(2):
            cs = slice(i * 1024, i * 1024 + 1024)
            a = jnp.dot(mix[r0 : r0 + CH, :], wobuf[:, cs], preferred_element_type=F32)
            a = a + xbuf[r0 : r0 + CH, cs].astype(F32)
            resid[:, cs] = a
            sq = a * a
            for b in range(8):
                ss = ss + sq[:, b * 128 : b * 128 + 128]
        rs = lax.rsqrt(jnp.sum(ss, axis=-1, keepdims=True) * (1.0 / D) + EPS)

        def norm(i, carry):
            cs = pl.ds(pl.multiple_of(i * 256, 256), 256)
            normed[HALO + r0 : HALO + r0 + CH, cs] = (resid[:, cs] * rs * fg_ref[:, cs]).astype(BF)
            return carry

        lax.fori_loop(0, 8, norm, 0)

        @pl.when(x == h)
        def _():
            def keep(i, carry):
                cs = pl.ds(pl.multiple_of(i * 256, 256), 256)
                own[:, cs] = resid[:, cs]
                return carry

            lax.fori_loop(0, 8, keep, 0)

    tail = normed.at[ROWS : ROWS + HALO, :]
    halo = normed.at[0:HALO, :]
    hcopy = remote(tail, halo, hsem.at[0], hsem.at[1], at_sp(spn))

    def norm_of(h):
        mwait(h, 2, xo)
        chunk_norm(h)

    norm_of(3)
    hcopy.start()
    norm_of(0)
    mrelay(1)
    wstep(1, 3)
    wstep(3, 0)
    mrelay(2)
    wstep(0, 4)
    norm_of(1)
    norm_of(2)
    wstep(2, 1)
    wstep(1, 4)
    hcopy.wait()

    @pl.when(sp == 0)
    def _():
        normed[0:HALO, :] = jnp.zeros((HALO, D), BF)

    for pc_ in range(2):
        for r in range(16):
            wpeer(pc_, r, peer).wait_recv()

    def up(i, h, mid=lambda: None):
        win = rows_of(h * CH, CH + HALO)

        def mixed_taps(u, taps):
            u = u.astype(BF).astype(F32)
            m = taps[0:1] * pltpu.roll(u, 2, 0) + taps[1:2] * pltpu.roll(u, 1, 0) + taps[2:3] * u
            return m[HALO:]

        def act(gm, vm):
            return (gm / (1.0 + jnp.exp(-gm)) * vm).astype(BF)

        for j in range(5):
            cs = slice(j * 256, j * 256 + 256)
            vs = slice(MAIN + j * 256, MAIN + j * 256 + 256)
            a = jnp.dot(normed[win, :], wgv[:, cs], preferred_element_type=F32)
            b = jnp.dot(normed[win, :], wgv[:, vs], preferred_element_type=F32)
            gm = mixed_taps(a, gt_ref[:, cs].astype(F32))
            vm = mixed_taps(b, vt_ref[:, cs].astype(F32))
            hid[i, :, cs] = act(gm, vm)
            if j == 2:
                mid()
        a = jnp.dot(normed[win, :], wgv[:, 2 * MAIN : GVW], preferred_element_type=F32)
        gm = mixed_taps(a[:, :128], gt_ref[:, MAIN:HID].astype(F32))
        vm = mixed_taps(a[:, 128:], vt_ref[:, MAIN:HID].astype(F32))
        hid[i, :, MAIN:HID] = act(gm, vm)

    def quarter(g):
        return slice(g * 512, g * 512 + 512)

    def down(i, g, add=False):
        a = jnp.dot(hid[i], dbuf[:, quarter(g)], preferred_element_type=F32)
        if add:
            a = a + relay[g].astype(F32)
        parts[i, :, quarter(g)] = a.astype(BF)

    def rs_copy(kind, g):
        if kind == 0:
            return remote(
                parts.at[0, :, quarter(g)], relay.at[g], psend.at[0, g], precv.at[0, g],
                dev(dx=xr if g in (0, 3) else xl),
            )
        return remote(
            parts.at[kind, :, quarter(g)], fin.at[kind - 1, :, quarter(g)], psend.at[kind, g],
            precv.at[kind, g], dev(dx=xr if kind == 1 else xl),
        )

    def dpeer(slots):
        for pc_ in (2, 3):
            for r in slots:
                wpeer(pc_, r, peer).wait_recv()

    def send_down(kind, g, relayed=False):
        if relayed:
            rs_copy(0, g).wait_recv()
        down(kind, g, relayed)
        rs_copy(kind, g).start()

    def first_sends():
        wstep(2, 2)
        wstep(3, 2)
        dpeer(range(1, 9))
        send_down(0, 0)
        send_down(0, 1)

    def third_quarter():
        wstep(3, 3)
        dpeer(range(9, 13))
        send_down(0, 2)

    up(0, xo, lambda: wstep(3, 1))
    up(1, xr, first_sends)
    send_down(1, 1)
    wstep(2, 3)
    up(2, xl, third_quarter)
    send_down(2, 0)
    send_down(1, 0, True)
    send_down(2, 1, True)
    wstep(2, 4)
    wstep(3, 4)
    dpeer(range(13, 16))
    send_down(0, 3)
    send_down(1, 2)
    send_down(2, 3)
    up(3, x)
    send_down(2, 2, True)
    for g in range(4):
        down(3, g)
    send_down(1, 3, True)

    for pc_ in range(4):
        for r in range(1, 16):
            wsendto(pc_, r).wait_send()
        for r in range(0 if pc_ < 2 else 1, 16):
            wpeer(pc_, r, c).wait_send()
    dx.wait_send()
    for cp in (o0, o1, o2, o3, *od, *ysent, *zsent, *msent):
        cp.wait_send()
    for g in (1, 0, 2, 3):
        rs_copy(1, g).wait_recv()
    for g in (0, 1, 3, 2):
        rs_copy(2, g).wait_recv()
    for s in range(16):
        zz, yy = shifted(OFF[s])
        cs = pl.ds(pl.multiple_of((zz * 4 + yy) * 128, 128), 128)
        ls = slice(s * 128, s * 128 + 128)
        a = own[:, cs] + parts[3, :, ls].astype(F32)
        a = a + (fin[0, :, ls].astype(F32) + fin[1, :, ls].astype(F32))
        out_ref[:, cs] = a.astype(BF)
    for kind in range(3):
        for g in range(4):
            rs_copy(kind, g).wait_send()


def per_device(
    residual_input_stream, projected_queries, projected_keys, projected_values,
    emitted_switch_entries, retention_preactivations, additional_fading_amount, head_norm_gain,
    attention_output_weight, feedforward_norm_gain, gate_up_matrix, value_up_matrix,
    gate_filter_taps, value_filter_taps, down_projection_weight,
):
    anyspec = pl.BlockSpec(memory_space=pl.ANY)
    vspec = pl.BlockSpec(memory_space=pltpu.VMEM)
    dma = pltpu.SemaphoreType.DMA
    v = pltpu.VMEM
    return pl.pallas_call(
        body,
        out_shape=jax.ShapeDtypeStruct((CH, D), BF),
        in_specs=[anyspec] * 10 + [vspec] * 5,
        out_specs=vspec,
        scratch_shapes=[
            v((D, GVW), BF), v((HID, D), BF), v((64, HID), BF), v((64, HID), BF),
            v((1024, D), BF), v((ROWS, D), BF),
            v((ROWS, 128), BF), v((ROWS, 128), BF), v((ROWS, 256), BF), v((ROWS, 256), BF),
            v((ROWS, 128), BF), v((ROWS, 128), F32), v((NB, 128, 128), F32), v((NB, 8, 128), F32),
            v((NB, 128, 128), BF), v((ROWS, 256), F32),
            v((2, 144, 128), BF), v((4, 144, 128), BF), v((4, 144, 128), BF),
            v((ROWS, 1024), BF), v((ROWS + HALO, D), BF), v((CH, D), F32), v((CH, D), F32),
            v((4, CH, HID), BF), v((4, CH, D), BF), v((4, CH, 512), BF), v((2, CH, D), BF),
            dma((12,)), dma((4, 16)), dma((4, 16)), dma((4, 16)), dma((4, 16)),
            dma((4,)), dma((4,)), dma((4,)), dma((4,)),
            dma((4,)), dma((3,)), dma((3,)), dma((3,)), dma((3,)),
            dma((4, 3)), dma((4, 3)), dma((2,)), dma((3, 4)), dma((3, 4)),
        ],
        compiler_params=pltpu.CompilerParams(
            collective_id=0, has_side_effects=True, vmem_limit_bytes=62 * 1024 * 1024
        ),
        name="layer",
    )(
        residual_input_stream, projected_queries, projected_keys, projected_values,
        emitted_switch_entries, retention_preactivations, attention_output_weight,
        gate_up_matrix, value_up_matrix, down_projection_weight.T,
        additional_fading_amount.reshape(ROWS // 128, 128), head_norm_gain[None],
        feedforward_norm_gain[None], gate_filter_taps, value_filter_taps,
    )


def solution(mesh):
    torus = Mesh(mesh.devices.reshape(4, 4, 2, mesh.shape["tp"]), (*SP, "tp"))
    return jax.shard_map(
        per_device,
        mesh=torus,
        in_specs=(
            P(SP, None), P(SP, "tp"), P(SP, "tp"), P(SP, "tp"), P(SP, "tp"), P(SP, "tp"),
            P(SP), P(), P("tp", None), P(), P(SP, "tp"), P(SP, "tp"), P(None, "tp"),
            P(None, "tp"), P("tp", SP),
        ),
        out_specs=P((*SP, "tp"), None),
        check_vma=False,
    )
```
